32 devices in a mesh: sp: 8 (over z, y), tp: 4 (over x, core).
Axes of the slice: x: 2, y: 2, z: 4, core: 2. Of those that a mesh axis runs over, the one named last changes fastest.
Arguments:
- hidden_activations: bfloat16 [6144, 4096], P(('sp', 'tp')), may hold values from -6 to 6
- entry_rescale_vector: bfloat16 [4096], replicated, may hold values from 0.099609375 to 1.8984375
- probe_matrix: bfloat16 [4096, 2048], P('sp', 'tp'), may hold values from -0.09375 to 0.09375
- lookup_address_matrix: bfloat16 [4096, 2048], P('sp', 'tp'), may hold values from -0.09375 to 0.09375
- payload_matrix: bfloat16 [4096, 4096], P('sp', 'tp'), may hold values from -0.09375 to 0.09375
- postfilter_switch_matrix: bfloat16 [4096, 4096], P('sp', 'tp'), may hold values from -0.09375 to 0.09375
- prefilter_switch_matrix: bfloat16 [4096, 4096], P('sp', 'tp'), may hold values from -0.09375 to 0.09375
- filter_source_matrix: bfloat16 [4096, 4096], P('sp', 'tp'), may hold values from -0.09375 to 0.09375
- forget_left_factor: bfloat16 [4096, 64], replicated, may hold values from -0.09375 to 0.09375
- forget_right_factor: bfloat16 [64, 2048], P(None, 'tp'), may hold values from -0.75 to 0.75
- forget_offset_per_feature: float32 [2048], P('tp'), may hold values from -1 to 12
- forget_spike_additions: float32 [16, 6144], P('tp', 'sp'), may hold values from -3 to 0
- subspace_rescale_vector: bfloat16 [16, 256], P('tp'), may hold values from 0.099609375 to 1.8984375
- depthwise_filter_taps: bfloat16 [3, 4096], P(None, 'tp'), may hold values from -3.5 to 3.5
- mixer_result_matrix: bfloat16 [4096, 4096], P('tp'), may hold values from -0.09375 to 0.09375
- filter_result_matrix: bfloat16 [4096, 4096], P('tp'), may hold values from -0.09375 to 0.09375
Outputs:
- mixed: bfloat16 [6144, 4096], P(('sp', 'tp'))
The draws below stay inside these ranges and needn't reach their ends.
All inputs are finite; a program needn't handle non-finite values.
Results may differ from the reference program's by a relative error of at most 0.02.
Values may be sent and summed in bfloat16 or wider, within the bound.
A program may use at most 128 MiB of HBM per device.

```python
import jax
import jax.numpy as jnp
from jax import lax

MODEL = 4096
HEAD_TOTAL = 16
KEY_CHANNELS = 128
VALUE_DIM = 256
CONV_DIM = 4096
DECAY_RANK = 64
TAPS = 3
BLOCK = 64
TOKENS_DEV = 768
TOKEN_LENGTH = 6144
KEY_WIDTH = 2048
VALUE_WIDTH = 4096
N_TP = 4


def draw_forget_offset_per_feature(key, part):
    key_slow = jax.random.fold_in(key, 11)
    key_fast = jax.random.fold_in(key, 12)
    key_pick = jax.random.fold_in(key, 13)
    slow_heads = jax.random.randint(key_pick, (HEAD_TOTAL,), 0, 10) < 5
    slow_values = jnp.log(TOKEN_LENGTH / 8.0) + jax.random.uniform(key_slow, (HEAD_TOTAL, KEY_CHANNELS), jnp.float32, -0.5, 0.5)
    fast_values = jax.random.uniform(key_fast, (HEAD_TOTAL, KEY_CHANNELS), jnp.float32, -0.5, 1.5)
    chosen = jnp.where(slow_heads[:, None], slow_values, fast_values)
    return chosen.reshape(HEAD_TOTAL * KEY_CHANNELS).astype(jnp.float32)


def draw_forget_spike_additions(key, part):
    key_rate = jax.random.fold_in(key, 21)
    key_where = jax.random.fold_in(key, 22)
    key_size = jax.random.fold_in(key, 23)
    block_total = TOKEN_LENGTH // TOKENS_DEV
    rates = jnp.exp(jax.random.uniform(key_rate, (HEAD_TOTAL, block_total), jnp.float32, jnp.log(0.05), jnp.log(0.4)))
    starting_figure = -jnp.repeat(rates / TOKEN_LENGTH, TOKENS_DEV, axis=1)
    where = jax.random.randint(key_where, (HEAD_TOTAL, 3), 0, TOKEN_LENGTH)
    extent_sequence = jnp.log(jax.random.uniform(key_size, (HEAD_TOTAL, 3), jnp.float32, 0.5, 0.8))
    positions = jnp.arange(TOKEN_LENGTH, dtype=jnp.int32)
    agreeing_tally = (positions[None, None, :] == where[:, :, None]).astype(jnp.float32)
    spike_amounts = jnp.sum(agreeing_tally * extent_sequence[:, :, None], axis=1)
    return (starting_figure + spike_amounts).astype(jnp.float32)


def levels(stream_key, extent, pieces, low, largest):
    factor_of = 1.0
    for position, parts in pieces:
        steps = jax.random.uniform(jax.random.fold_in(jax.random.fold_in(stream_key, 6), position), (parts,), jnp.float32, low / len(pieces), largest / len(pieces))
        factor_of = factor_of * jnp.repeat(jnp.exp(steps), extent[position] // parts).reshape((-1,) + (1,) * (len(extent) - 1 - position))
    return factor_of


def scatter_about(key, shape, spread, bound, pieces=(), kind=jnp.bfloat16):
    level = levels(key, shape, pieces, -0.22, 0.18) if pieces else 1.0
    drawn = jax.random.normal(key, shape, jnp.float32) * spread * level
    return jnp.minimum(jnp.maximum(drawn, -bound), bound).astype(kind)


def setup_inputs(seed: int = 0) -> dict:
    key_of = jax.random.split(jax.random.key(seed), 17)
    return {
        "hidden_activations": scatter_about(key_of[0], (TOKEN_LENGTH, MODEL), 1.0, 6.0, ((0, 32),)),
        "entry_rescale_vector": jnp.clip(1.0 + 0.18 * jax.random.normal(key_of[1], (MODEL,), jnp.float32), 0.099609375, 1.8984375).astype(jnp.bfloat16),
        "probe_matrix": scatter_about(key_of[2], (MODEL, KEY_WIDTH), MODEL ** -0.5, 0.09375, ((0, 8), (1, 4))),
        "lookup_address_matrix": scatter_about(key_of[3], (MODEL, KEY_WIDTH), MODEL ** -0.5, 0.09375, ((0, 8), (1, 4))),
        "payload_matrix": scatter_about(key_of[4], (MODEL, VALUE_WIDTH), MODEL ** -0.5, 0.09375, ((0, 8), (1, 4))),
        "postfilter_switch_matrix": scatter_about(key_of[5], (MODEL, CONV_DIM), MODEL ** -0.5, 0.09375, ((0, 8), (1, 4))),
        "prefilter_switch_matrix": scatter_about(key_of[6], (MODEL, CONV_DIM), MODEL ** -0.5, 0.09375, ((0, 8), (1, 4))),
        "filter_source_matrix": scatter_about(key_of[7], (MODEL, CONV_DIM), MODEL ** -0.5, 0.09375, ((0, 8), (1, 4))),
        "forget_left_factor": scatter_about(key_of[8], (MODEL, DECAY_RANK), MODEL ** -0.5, 0.09375),
        "forget_right_factor": scatter_about(key_of[9], (DECAY_RANK, KEY_WIDTH), DECAY_RANK ** -0.5, 0.75, ((1, 4),)),
        "forget_offset_per_feature": draw_forget_offset_per_feature(jax.random.fold_in(key_of[16], 71), 0),
        "forget_spike_additions": draw_forget_spike_additions(jax.random.fold_in(key_of[16], 71), 0),
        "subspace_rescale_vector": jnp.clip(1.0 + 0.18 * jax.random.normal(key_of[12], (HEAD_TOTAL, VALUE_DIM), jnp.float32), 0.099609375, 1.8984375).astype(jnp.bfloat16),
        "depthwise_filter_taps": scatter_about(key_of[13], (TAPS, CONV_DIM), TAPS ** -0.5, 3.5, ((1, 4),)),
        "mixer_result_matrix": scatter_about(key_of[14], (VALUE_WIDTH, MODEL), VALUE_WIDTH ** -0.5, 0.09375, ((0, 4),)),
        "filter_result_matrix": scatter_about(key_of[15], (CONV_DIM, MODEL), CONV_DIM ** -0.5, 0.09375, ((0, 4),)),
    }


epsilon = 1e-06
softness_scale = 16.0

def row_norm(rows, gain):
    rows_f = rows.astype(jnp.float32)
    meansq = lax.optimization_barrier(jnp.mean(rows_f * rows_f, axis=-1, keepdims=True))
    return rows_f * lax.rsqrt(meansq + epsilon) * gain.astype(jnp.float32)

def block_terms(query_rows, key_rows, value_rows, forget_log_rate):
    length_value, head_number, key_dim = query_rows.shape
    value_dim = value_rows.shape[2]
    block_count = length_value // BLOCK
    key_shape = (block_count, BLOCK, head_number, key_dim)
    query_f32 = query_rows.astype(jnp.float32).reshape(key_shape) * key_dim ** (-0.5)
    key_f32 = key_rows.astype(jnp.float32).reshape(key_shape)
    value_f32 = value_rows.astype(jnp.float32).reshape(block_count, BLOCK, head_number, value_dim)
    within = jnp.cumsum(forget_log_rate.reshape(key_shape), axis=1)
    block_end = within[:, -1]
    query_decayed = query_f32 * jnp.exp(within)
    key_inverse = key_f32 * jnp.exp(-within)
    key_tail = key_f32 * jnp.exp(block_end[:, None] - within)
    highest = lax.Precision.HIGHEST
    scores = jnp.einsum('nihd,njhd->nhij', query_decayed, key_inverse, precision=highest)
    causal = jnp.tril(jnp.ones((BLOCK, BLOCK), dtype=bool))
    scores = jnp.where(causal, scores, 0.0)
    inside = jnp.einsum('nhij,njhv->nihv', scores, value_f32, precision=highest)
    updates = jnp.einsum('njhd,njhv->nhdv', key_tail, value_f32, precision=highest)

    def advance(state, pair):
        decay_now, update_now = pair
        return (jnp.exp(decay_now)[..., None] * state + update_now, state)
    start_state = jnp.zeros((head_number, key_dim, value_dim), jnp.float32)
    final_state, state_in = lax.scan(advance, start_state, (block_end, updates))
    carried = jnp.einsum('nihd,nhdv->nihv', query_decayed, state_in, precision=highest)
    return (inside + carried, query_decayed, block_end, final_state)

def reference(hidden_activations, entry_rescale_vector, probe_matrix, lookup_address_matrix, payload_matrix, postfilter_switch_matrix, prefilter_switch_matrix, filter_source_matrix, forget_left_factor, forget_right_factor, forget_offset_per_feature, forget_spike_additions, subspace_rescale_vector, depthwise_filter_taps, mixer_result_matrix, filter_result_matrix):
    normalized_input = row_norm(hidden_activations, entry_rescale_vector).astype(jnp.bfloat16)

    def project(weight):
        return jnp.dot(normalized_input, weight, preferred_element_type=jnp.float32).astype(jnp.bfloat16)
    queries = project(probe_matrix)
    key_rows = project(lookup_address_matrix)
    value_rows = project(payload_matrix)
    outer = project(postfilter_switch_matrix)
    inner = project(prefilter_switch_matrix)
    conv_in = project(filter_source_matrix)
    low_rank = project(forget_left_factor)
    gate_preactivation = jnp.dot(low_rank, forget_right_factor, preferred_element_type=jnp.float32) + forget_offset_per_feature
    forget_log_rate = (jax.nn.log_sigmoid(gate_preactivation) / softness_scale).reshape(TOKEN_LENGTH, HEAD_TOTAL, KEY_CHANNELS)
    forget_log_rate = forget_log_rate + jnp.transpose(forget_spike_additions)[:, :, None]
    attended, unused_q, unused_e, unused_s = block_terms(queries.reshape(TOKEN_LENGTH, HEAD_TOTAL, KEY_CHANNELS), key_rows.reshape(TOKEN_LENGTH, HEAD_TOTAL, KEY_CHANNELS), value_rows.reshape(TOKEN_LENGTH, HEAD_TOTAL, VALUE_DIM), forget_log_rate)
    attended = attended.reshape(TOKEN_LENGTH, HEAD_TOTAL, VALUE_DIM)
    mixed_attn = row_norm(attended, subspace_rescale_vector).astype(jnp.bfloat16).reshape(TOKEN_LENGTH, HEAD_TOTAL * VALUE_DIM)
    gated_in = (inner.astype(jnp.float32) * conv_in.astype(jnp.float32)).astype(jnp.bfloat16)
    padded = jnp.concatenate([jnp.zeros((TAPS - 1, CONV_DIM), jnp.bfloat16), gated_in], axis=0)
    taps_f32 = depthwise_filter_taps.astype(jnp.float32)
    conv_sum = jnp.zeros((TOKEN_LENGTH, CONV_DIM), jnp.float32)
    for tap_index in range(TAPS):
        conv_sum = conv_sum + taps_f32[tap_index] * padded[tap_index:tap_index + TOKEN_LENGTH].astype(jnp.float32)
    mixed_conv = (conv_sum * outer.astype(jnp.float32)).astype(jnp.bfloat16)
    head_cols = HEAD_TOTAL * VALUE_DIM // N_TP
    conv_cols = CONV_DIM // N_TP
    running = jnp.zeros((TOKEN_LENGTH, MODEL), jnp.float32)
    for group in range(N_TP):
        term = jnp.dot(mixed_attn[:, group * head_cols:(group + 1) * head_cols], mixer_result_matrix[group * head_cols:(group + 1) * head_cols], preferred_element_type=jnp.float32)
        term = term + jnp.dot(mixed_conv[:, group * conv_cols:(group + 1) * conv_cols], filter_result_matrix[group * conv_cols:(group + 1) * conv_cols], preferred_element_type=jnp.float32)
        rounded = lax.optimization_barrier(term.astype(jnp.bfloat16))
        running = running + rounded.astype(jnp.float32)
    return running.astype(jnp.bfloat16)
```

```python
import functools

import jax
import jax.numpy as jnp
from jax import lax
from jax.sharding import PartitionSpec as P

BLOCK = 64


epsilon = 1e-06
softness_scale = 16.0


def entering(shard, axis, join, neutral):
    place = lax.axis_index(axis)
    gathered = jax.tree.map(
        lambda a, kind: lax.all_gather(a.astype(kind), axis), shard, (jnp.bfloat16, jnp.bfloat16)
    )
    state = jax.tree.map(lambda a, e: jnp.zeros_like(a) + jnp.asarray(e, a.dtype), shard, neutral)

    def one(lap, state):
        return join(
            state,
            jax.tree.map(
                lambda a, own: lax.dynamic_index_in_dim(a, lap, 0, False).astype(own.dtype),
                gathered,
                shard,
            ),
        )

    return lax.fori_loop(0, place, one, state)


def shifted(value, axis, steps):
    count = lax.axis_size(axis)
    leading, last = (max(0, -steps), min(count, count - steps))
    return lax.ppermute(value, axis, [(source, source + steps) for source in range(leading, last)])


def norm_values(rows, gain):
    rows_f = rows.astype(jnp.float32)
    meansq = jnp.mean(rows_f * rows_f, axis=-1, keepdims=True)
    return rows_f * lax.rsqrt(meansq + epsilon) * gain.astype(jnp.float32)


def row_norm(gain, rows):
    return norm_values(rows, gain).astype(jnp.bfloat16)


def ring_order(mesh):
    line = mesh.devices[:, 0]
    count = len(line)
    try:
        first = tuple(line[0].coords)
        width = sum(1 for d in line if d.coords[2] == first[2])
    except Exception:
        return tuple(range(count))
    tall = count // width
    if width * tall != count or tall % 2:
        return tuple(range(count))
    if width == 1:
        return tuple(range(count))
    path = []
    for z in range(tall):
        columns = range(1, width) if z % 2 == 0 else range(width - 1, 0, -1)
        path += [z * width + y for y in columns]
    path += [z * width for z in range(tall - 1, -1, -1)]
    return tuple(path)


def ring_project(order, normalized_input, weight, hold=None):
    count = len(order)
    rows = weight.shape[0]
    half = rows // 2
    length = normalized_input.shape[0]
    owners = jnp.asarray(order, jnp.int32)
    place = jnp.asarray([order.index(i) for i in range(count)], jnp.int32)[lax.axis_index("sp")]
    ahead = [(order[i], order[(i + 1) % count]) for i in range(count)]
    behind = [(target, source) for source, target in ahead]
    top, low = weight[:half], weight[half:]
    held = hold is not None
    if held:
        top, low, hold = lax.optimization_barrier((top, low, hold))

    def product(first, second, upper, lower):
        left = jnp.concatenate(
            [
                lax.dynamic_slice(normalized_input, (jnp.int32(0), at), (length, half))
                for at in (first * rows, second * rows + half)
            ],
            axis=1,
        )
        block = jnp.concatenate([upper, lower], axis=0)
        return jnp.dot(left, block, preferred_element_type=jnp.float32)

    pending = [(owners[place], owners[place], top, low)]
    total = jnp.zeros((length, weight.shape[1]), jnp.float32)
    for step in range(1, count):
        top = lax.ppermute(top, "sp", ahead)
        low = lax.ppermute(low, "sp", behind)
        for entry in pending:
            total = total + product(*entry)
        if held:
            top, low, total = lax.optimization_barrier((top, low, total))
        pending = [
            (
                owners[lax.rem(place - step + count, count)],
                owners[lax.rem(place + step, count)],
                top,
                low,
            )
        ]
    return total, pending, product, hold


def ring_finish(total, pending, product):
    for entry in pending:
        total = total + product(*entry)
    return total


def block_terms(query_rows, key_rows, value_rows, forget_log_rate):
    length_value, head_number, key_dim = query_rows.shape
    value_dim = value_rows.shape[2]
    block_count = length_value // BLOCK
    key_shape = (block_count, BLOCK, head_number, key_dim)
    query_f32 = query_rows.astype(jnp.float32).reshape(key_shape) * key_dim ** (-0.5)
    key_f32 = key_rows.astype(jnp.float32).reshape(key_shape)
    value_f32 = value_rows.astype(jnp.float32).reshape(block_count, BLOCK, head_number, value_dim)
    within = jnp.cumsum(forget_log_rate.reshape(key_shape), axis=1)
    block_end = within[:, -1]
    query_decayed = query_f32 * jnp.exp(within)
    key_inverse = key_f32 * jnp.exp(-within)
    key_tail = key_f32 * jnp.exp(block_end[:, None] - within)
    highest = lax.Precision.HIGHEST
    scores = jnp.einsum("nihd,njhd->nhij", query_decayed, key_inverse, precision=highest)
    causal = jnp.tril(jnp.ones((BLOCK, BLOCK), dtype=bool))
    scores = jnp.where(causal, scores, 0.0)
    inside = jnp.einsum("nhij,njhv->nihv", scores, value_f32, precision=highest)
    updates = jnp.einsum("njhd,njhv->nhdv", key_tail, value_f32, precision=highest)

    def advance(state, pair):
        decay_now, update_now = pair
        return (jnp.exp(decay_now)[..., None] * state + update_now, state)

    start_state = jnp.zeros((head_number, key_dim, value_dim), jnp.float32)
    final_state, state_in = lax.scan(advance, start_state, (block_end, updates))
    carried = jnp.einsum("nihd,nhdv->nihv", query_decayed, state_in, precision=highest)
    return (inside + carried, query_decayed, block_end, final_state)


def chain_combine(earlier, later):
    return (earlier[0] * later[0], later[0][..., None] * earlier[1] + later[1])


def attention_path(
    normalized_input,
    sum_values,
    forget_left_factor,
    forget_right_factor,
    forget_offset_per_feature,
    forget_spike_additions,
    subspace_rescale_vector,
):
    length_value = normalized_input.shape[0]
    head_number = subspace_rescale_vector.shape[0]
    value_dim = subspace_rescale_vector.shape[1]
    query_rows = sum_values[0].astype(jnp.bfloat16).reshape(length_value, head_number, -1)
    key_rows = sum_values[1].astype(jnp.bfloat16).reshape(length_value, head_number, -1)
    value_rows = sum_values[2].astype(jnp.bfloat16).reshape(length_value, head_number, value_dim)
    low_rank = jnp.dot(
        normalized_input, forget_left_factor, preferred_element_type=jnp.float32
    ).astype(jnp.bfloat16)
    gate_preactivation = (
        jnp.dot(low_rank, forget_right_factor, preferred_element_type=jnp.float32)
        + forget_offset_per_feature
    )
    forget_log_rate = (jax.nn.log_sigmoid(gate_preactivation) / softness_scale).reshape(
        length_value, head_number, -1
    )
    forget_log_rate = forget_log_rate + jnp.transpose(forget_spike_additions)[:, :, None]
    local_out, query_decayed, block_end, final_state = block_terms(
        query_rows, key_rows, value_rows, forget_log_rate
    )
    prefix = jnp.cumsum(block_end, axis=0) - block_end
    query_far = query_decayed * jnp.exp(prefix)[:, None]
    total_decay = jnp.exp(jnp.sum(block_end, axis=0))
    identity = (jnp.ones_like(total_decay), jnp.zeros_like(final_state))
    incoming = entering((total_decay, final_state), "sp", chain_combine, identity)[1]
    attended = local_out + jnp.einsum(
        "nihd,hdv->nihv", query_far, incoming, precision=lax.Precision.HIGHEST
    )
    attended = attended.reshape(length_value, head_number, value_dim)
    return (
        norm_values(attended, subspace_rescale_vector)
        .astype(jnp.bfloat16)
        .reshape(length_value, head_number * value_dim)
    )


def conv_branch(sum_values, depthwise_filter_taps):
    outer = sum_values[0].astype(jnp.bfloat16)
    inner = sum_values[1].astype(jnp.bfloat16)
    conv_in = sum_values[2].astype(jnp.bfloat16)
    length_value = outer.shape[0]
    gated_in = (inner.astype(jnp.float32) * conv_in.astype(jnp.float32)).astype(jnp.bfloat16)
    reach = depthwise_filter_taps.shape[0] - 1
    rim_rows = shifted(gated_in[length_value - reach :], "sp", 1)
    padded = jnp.concatenate([rim_rows, gated_in], axis=0)
    taps_f32 = depthwise_filter_taps.astype(jnp.float32)
    conv_sum = jnp.zeros(outer.shape, jnp.float32)
    for tap_index in range(depthwise_filter_taps.shape[0]):
        conv_sum = conv_sum + taps_f32[tap_index] * padded[
            tap_index : tap_index + length_value
        ].astype(jnp.float32)
    return (conv_sum * outer.astype(jnp.float32)).astype(jnp.bfloat16)


def body(
    order,
    hidden_activations,
    entry_rescale_vector,
    probe_matrix,
    lookup_address_matrix,
    payload_matrix,
    postfilter_switch_matrix,
    prefilter_switch_matrix,
    filter_source_matrix,
    forget_left_factor,
    forget_right_factor,
    forget_offset_per_feature,
    forget_spike_additions,
    subspace_rescale_vector,
    depthwise_filter_taps,
    mixer_result_matrix,
    filter_result_matrix,
):
    normalized_input = row_norm(
        entry_rescale_vector, lax.all_gather(hidden_activations, "tp", axis=0, tiled=True)
    )
    attn_weights = (probe_matrix, lookup_address_matrix, payload_matrix)
    conv_weights = (postfilter_switch_matrix, prefilter_switch_matrix, filter_source_matrix)

    def parts(total, weights):
        edges = [0]
        for weight in weights:
            edges.append(edges[-1] + weight.shape[1])
        return [total[:, i:j] for i, j in zip(edges[:-1], edges[1:])]

    attn_total, attn_last, attn_product, _ = ring_project(
        order, normalized_input, jnp.concatenate(attn_weights, axis=1)
    )
    conv_total, conv_last, conv_product, attn_total = ring_project(
        order, normalized_input, jnp.concatenate(conv_weights, axis=1), attn_total
    )
    attn_total = ring_finish(attn_total, attn_last, attn_product)
    conv_total = ring_finish(conv_total, conv_last, conv_product)
    every_sum = parts(attn_total, attn_weights) + parts(conv_total, conv_weights)
    mixed_attn = attention_path(
        normalized_input,
        every_sum[:3],
        forget_left_factor,
        forget_right_factor,
        forget_offset_per_feature,
        forget_spike_additions,
        subspace_rescale_vector,
    )
    mixed_conv = conv_branch(every_sum[3:], depthwise_filter_taps)
    return lax.psum_scatter(
        (
            jnp.dot(mixed_attn, mixer_result_matrix, preferred_element_type=jnp.float32)
            + jnp.dot(mixed_conv, filter_result_matrix, preferred_element_type=jnp.float32)
        ).astype(jnp.bfloat16),
        "tp",
        scatter_dimension=0,
        tiled=True,
    )


def solution(mesh):
    in_specs = (
        P(("sp", "tp"), None),
        P(),
        P("sp", "tp"),
        P("sp", "tp"),
        P("sp", "tp"),
        P("sp", "tp"),
        P("sp", "tp"),
        P("sp", "tp"),
        P(),
        P(None, "tp"),
        P("tp"),
        P("tp", "sp"),
        P("tp", None),
        P(None, "tp"),
        P("tp", None),
        P("tp", None),
    )
    out_specs = P(("sp", "tp"), None)
    return jax.shard_map(functools.partial(body, ring_order(mesh)), mesh=mesh, in_specs=in_specs, out_specs=out_specs, check_vma=False)
```
